32 devices in a mesh: sp: 8 (over z, y), tp: 4 (over x, core).
Axes of the slice: x: 2, y: 2, z: 4, core: 2. Of those that a mesh axis runs over, the one named last changes fastest.
Arguments:
- out_cotangent: bfloat16 [1024, 2048], P('sp'), may hold values from -6 to 6
- routes: int32 [1024, 2], P('sp'), may hold values from 0 to 7, all different within a row; in each aligned block of 128 rows (0 to 127, 128 to 255, ...) at most 48 rows name the same one
- route_weights: float32 [1024, 2], P('sp'), may hold values from 0.3 to 1.5
- expert_rows: bfloat16 [8, 384, 2048], P('sp', None, 'tp'), may hold values from -6 to 6
- w_gate: bfloat16 [8, 2048, 1024], P('sp', None, 'tp'), may hold values from -0.125 to 0.125
- w_up: bfloat16 [8, 2048, 1024], P('sp', None, 'tp'), may hold values from -0.125 to 0.125
- w_down: bfloat16 [8, 1024, 2048], P('sp', 'tp'), may hold values from -0.1875 to 0.1875
- out_weight: bfloat16 [2048, 4096], P('sp', 'tp'), may hold values from -0.09375 to 0.09375
- values: bfloat16 [1024, 4096], P('sp', 'tp'), may hold values from -0.75 to 0.75
- keys: bfloat16 [1024, 1024], P('sp', 'tp'), may hold values from -0.5 to 0.5
- queries: bfloat16 [1024, 1024], P('sp', 'tp'), may hold values from -6 to 6
- log_decay: float32 [1024, 64], P('sp', 'tp'), may hold values from -1 to 0
- gate_input: bfloat16 [1024, 4096], P('sp', 'tp'), may hold values from -6 to 6
Outputs:
- grad_w_gate: bfloat16 [8, 2048, 1024], P('sp', None, 'tp')
- grad_w_up: bfloat16 [8, 2048, 1024], P('sp', None, 'tp')
- grad_w_down: bfloat16 [8, 1024, 2048], P('sp', 'tp')
- grad_out_weight: float32 [2048, 4096], P('sp', 'tp')
- grad_residual: float32 [1024, 2048], P('sp', 'tp')
- grad_values: float32 [1024, 4096], P('sp', 'tp')
- grad_keys: float32 [1024, 1024], P('sp', 'tp')
- grad_queries: float32 [1024, 1024], P('sp', 'tp')
- grad_decay: float32 [1024, 64], P('sp', 'tp')
- grad_gate: float32 [1024, 4096], P('sp', 'tp')
The draws below stay inside these ranges and needn't reach their ends.
Inputs may be any that keep to these rules, and one draw needn't show every extreme that they name: `routes`: in each aligned block of 128 tokens no expert is named by more than 48 pairs, a bound that some block reaches.
All inputs are finite; a program needn't handle non-finite values.
Results may differ from the reference program's by a relative error of at most 0.0062.
Values may be sent and summed in bfloat16 or wider, within the bound.
No kernel may reach another device: no remote copies, remote signals or barrier semaphores. Data moves between devices by JAX's collectives and lax.ppermute only.
A program may use at most 128 MiB of HBM per device.

```python
import math
import jax
import jax.numpy as jnp
import numpy as np
from jax import lax

D = 2048
MIXER_HEADS = 64
HEAD_DIM = 64
GROUPS = 8
STATE = 128
INNER = 4096
EXPERT_FF = 1024
EXPERTS = 8
TOP = 2
TOK_DEV = 128
SPAN = 128
SEQUENCE_TOKENS = 1024
CAP = 48
SLOTS = 384
N_SP = 8


def draw_log_decay(key, part):
    parallel_flows = jax.random.split(jax.random.fold_in(key, 11), 6)
    quick_decay_heads = (jax.random.randint(parallel_flows[0], (MIXER_HEADS,), 0, 2) == 1).astype(jnp.float32)
    fast_rate = jax.random.uniform(parallel_flows[1], (MIXER_HEADS,), jnp.float32, 1.0 / 90.0, 1.0 / 30.0)
    slow_rate = 0.4 / SEQUENCE_TOKENS
    base_rate = quick_decay_heads * fast_rate + (1.0 - quick_decay_heads) * slow_rate
    device_count = SEQUENCE_TOKENS // TOK_DEV
    device_scale = jnp.exp(jax.random.uniform(parallel_flows[2], (device_count,), jnp.float32, -0.7, 0.7))
    position_scale = jnp.repeat(device_scale, TOK_DEV)
    rough = jax.random.uniform(parallel_flows[3], (SEQUENCE_TOKENS, MIXER_HEADS), jnp.float32, 0.4, 1.6)
    decay_rates = base_rate[None, :] * position_scale[:, None] * rough
    spike_position = jax.random.randint(parallel_flows[4], (2,), 0, SEQUENCE_TOKENS)
    spike_length = jnp.log(jax.random.uniform(parallel_flows[5], (2, MIXER_HEADS), jnp.float32, 0.5, 0.8))
    spike_matches = (jnp.arange(SEQUENCE_TOKENS)[:, None] == spike_position[None, :]).astype(jnp.float32)
    spike_groups = jnp.dot(spike_matches, spike_length) * (1.0 - quick_decay_heads)[None, :]
    return (spike_groups - decay_rates).astype(jnp.float32)


def with_spikes(entries, stream_key, source, target, blocks, factor):
    def block_of(axis_at):
        return (jnp.arange(entries.shape[axis_at]) // (entries.shape[axis_at] // blocks)).reshape((-1,) + (1,) * (entries.ndim - 1 - axis_at))

    near = jax.random.permutation(stream_key, blocks)[block_of(target)]
    other_side = (block_of(target) + blocks // 2) % blocks
    return jnp.where((block_of(source) == near) | (block_of(source) == other_side), factor * entries, entries)


def levels(own_key, dims, cuts, low, largest):
    def one(axis_at, parts):
        draws = jax.random.uniform(jax.random.fold_in(jax.random.fold_in(own_key, 6), axis_at), (parts,), jnp.float32, low / len(cuts), largest / len(cuts))
        return jnp.repeat(jnp.exp(draws), dims[axis_at] // parts).reshape((-1,) + (1,) * (len(dims) - axis_at - 1))

    gain = one(*cuts[0])
    for cut in cuts[1:]:
        gain = gain * one(*cut)
    return gain


def routed_block(stream_key, own, number, rows, count, top, bound, skew):
    order = jax.random.permutation(stream_key, count)
    heavy_load, ordinary = shares(count, rows * top, bound, skew, True), shares(count, rows * top, bound, skew, False)
    places = jnp.arange(count)

    def named(tallies, rotation):
        used = int((tallies > 0).sum())
        fixed = max(1, used // 4)
        shifted = fixed + (places - fixed + rotation * (used - fixed)) % max(1, count - fixed)
        return jnp.zeros((count,), jnp.int32).at[order[jnp.where(places < fixed, places, shifted)]].set(jnp.asarray(tallies, jnp.int32))

    tallies = jnp.where(number % 4 == 0, named(heavy_load, number // 4), named(ordinary, number - number // 4 - 1))
    mixed = jax.random.permutation(jax.random.fold_in(own, 3), count)
    giver, taker = mixed[0:count // 2 * 2:2], mixed[1:count // 2 * 2:2]
    margin = jnp.minimum(tallies[giver] - 1, bound - tallies[taker]) // 2
    margin = jnp.where((giver == order[0]) | (taker == order[0]) | (tallies[taker] == 0), 0, jnp.maximum(margin, 0))
    shifted = jax.random.randint(jax.random.fold_in(own, 4), (count // 2,), 0, 1 << 20) % (margin + 1)
    tallies = tallies.at[giver].add(-shifted).at[taker].add(shifted)
    labels = jnp.searchsorted(jnp.cumsum(tallies), jnp.arange(rows * top), side="right").astype(jnp.int32)
    table = labels.reshape(top, rows).T
    table = table[jax.random.permutation(jax.random.fold_in(own, 1), rows)]
    rotation = jax.random.randint(jax.random.fold_in(own, 2), (rows, 1), 0, top)
    return jnp.take_along_axis(table, (jnp.arange(top)[None, :] + rotation) % top, axis=1)


def shares(count, total, reach, skew, full):
    portions = [(1 << 20) // math.isqrt(rank ** skew) + 1 for rank in range(1, count + 1)]
    largest = reach if full else min(reach, max(-(-total // count), total * portions[0] // sum(portions)))
    least = 1 if total - largest >= count - 1 else 0
    given, spare = [largest] + [least] * (count - 1), total - largest - least * (count - 1)
    while spare > 0:
        free = [i for i in range(1, count) if given[i] < largest] or [i for i in range(1, count) if given[i] < reach]
        mass, budget = sum([portions[i] for i in free]), spare
        for i in free:
            addition = min(reach - given[i], max(1, budget * portions[i] // mass), spare)
            given[i] = given[i] + addition
            spare = spare - addition
    return np.array(given)


def bell_draw(own_key, shape, deviation, limit, shards=(), kind=jnp.bfloat16):
    result = jax.random.normal(own_key, shape, jnp.float32) * deviation
    if len(shards) > 0:
        result = levels(own_key, shape, shards, -0.22, 0.18) * result
    return jnp.clip(result, min=-limit, max=limit).astype(kind)


def heavy_noise(key, shape, width, bound, cuts, heavy, kind=jnp.bfloat16):
    array = width * jax.random.normal(key, shape, jnp.float32)
    if cuts:
        array = array * levels(key, shape, cuts, -0.22, 0.18)
    return jnp.clip(with_spikes(array, jax.random.fold_in(key, 3), *heavy), -bound, bound).astype(kind)


def setup_inputs(seed: int = 0) -> dict:
    seeds = jax.random.split(jax.random.key(seed), 14)
    out_cotangent = heavy_noise(seeds[0], (SEQUENCE_TOKENS, D), 1.0, 6.0, ((0, 8),), (0, 1, 8, 2.0))
    routes_keys = jax.random.split(jax.random.fold_in(seeds[1], 1), SEQUENCE_TOKENS // TOK_DEV)
    routes_turns = jax.random.permutation(jax.random.fold_in(seeds[1], 3), SEQUENCE_TOKENS // TOK_DEV)
    routes = jax.vmap(lambda own, number: routed_block(jax.random.fold_in(seeds[1], 2), own, number, TOK_DEV, EXPERTS, TOP, CAP, 2))(routes_keys, routes_turns).reshape((SEQUENCE_TOKENS, TOP))
    route_weights = jnp.clip(0.3 + 1.2 * jax.random.uniform(seeds[2], (SEQUENCE_TOKENS, TOP), jnp.float32) ** levels(seeds[2], (SEQUENCE_TOKENS, TOP), ((0, 8),), -0.2, 0.2), 0.3, 1.5)
    expert_rows = bell_draw(seeds[3], (EXPERTS, SLOTS, D), 1.0, 6.0, ((0, 8), (2, 4)))
    w_gate = bell_draw(seeds[4], (EXPERTS, D, EXPERT_FF), D ** -0.5, 0.125, ((0, 8), (2, 4)))
    w_up = bell_draw(seeds[5], (EXPERTS, D, EXPERT_FF), D ** -0.5, 0.125, ((0, 8), (2, 4)))
    w_down = bell_draw(seeds[6], (EXPERTS, EXPERT_FF, D), EXPERT_FF ** -0.5, 0.1875, ((0, 8), (1, 4)))
    out_weight = bell_draw(seeds[7], (D, INNER), INNER ** -0.5, 0.09375, ((0, 8), (1, 4)))
    values = bell_draw(seeds[8], (SEQUENCE_TOKENS, INNER), (SEQUENCE_TOKENS // 16) ** -0.5, 0.75, ((0, 8), (1, 4)))
    keys = bell_draw(seeds[9], (SEQUENCE_TOKENS, GROUPS * STATE), STATE ** -0.5, 0.5, ((0, 8), (1, 4)))
    queries = bell_draw(seeds[10], (SEQUENCE_TOKENS, GROUPS * STATE), 1.0, 6.0, ((0, 8), (1, 4)))
    log_decay = draw_log_decay(jax.random.fold_in(seeds[13], 71), 0)
    gate_input = bell_draw(seeds[12], (SEQUENCE_TOKENS, INNER), 1.0, 6.0, ((0, 8), (1, 4)))
    return {"out_cotangent": out_cotangent, "routes": routes, "route_weights": route_weights, "expert_rows": expert_rows, "w_gate": w_gate, "w_up": w_up, "w_down": w_down, "out_weight": out_weight, "values": values, "keys": keys, "queries": queries, "log_decay": log_decay, "gate_input": gate_input}


HIGHEST = lax.Precision.HIGHEST

def block_step(state_now, block_input):
    values_blk, keys_blk, queries_blk, decay_blk = block_input
    span_len, head_count, head_dim = values_blk.shape
    groups = keys_blk.shape[1]
    state_dim = keys_blk.shape[2]
    repeat = head_count // groups
    cumulative = jnp.cumsum(decay_blk, axis=0)
    lower_mask = jnp.arange(span_len)[:, None] >= jnp.arange(span_len)[None, :]
    segment = cumulative[:, None, :] - cumulative[None, :, :]
    weights = jnp.exp(jnp.where(lower_mask[:, :, None], segment, -jnp.inf)).reshape(span_len, span_len, groups, repeat)
    inner_prod = jnp.einsum('tgn,sgn->tsg', queries_blk, keys_blk, precision=HIGHEST)
    grouped = values_blk.reshape(span_len, groups, repeat, head_dim)
    combined = inner_prod[:, :, :, None] * weights
    within = jnp.einsum('tsgr,sgrp->tgrp', combined, grouped, precision=HIGHEST)
    carried = jnp.einsum('tgn,grpn->tgrp', queries_blk, state_now.reshape(groups, repeat, head_dim, state_dim), precision=HIGHEST)
    carried = carried * jnp.exp(cumulative).reshape(span_len, groups, repeat)[..., None]
    to_end = jnp.exp(cumulative[-1][None, :] - cumulative).reshape(span_len, groups, repeat)
    added_state = jnp.einsum('sgn,sgrp->grpn', keys_blk, grouped * to_end[..., None], precision=HIGHEST)
    new_state = state_now * jnp.exp(cumulative[-1])[:, None, None] + added_state.reshape(head_count, head_dim, state_dim)
    return (new_state, (within + carried).reshape(span_len, head_count * head_dim))

def mixer_scan(value_f, key_f, query_f, decay_f, start_state):
    row_count = value_f.shape[0]
    head_count = decay_f.shape[1]
    groups = key_f.shape[1] // STATE
    head_dim = value_f.shape[1] // head_count
    span_len = min(SPAN, row_count)
    blocks = row_count // span_len
    value_b = value_f.reshape(blocks, span_len, head_count, head_dim)
    key_b = key_f.reshape(blocks, span_len, groups, STATE)
    query_b = query_f.reshape(blocks, span_len, groups, STATE)
    decay_b = decay_f.reshape(blocks, span_len, head_count)
    end_state, outputs = lax.scan(block_step, start_state, (value_b, key_b, query_b, decay_b))
    return (outputs.reshape(row_count, head_count * head_dim), end_state)

def expert_backward(expert_item):
    saved, grads_in, gate_w, up_w, down_w = expert_item
    gate_pre = jnp.dot(saved, gate_w, preferred_element_type=jnp.float32)
    up_pre = jnp.dot(saved, up_w, preferred_element_type=jnp.float32)
    sigmoid_gate = jax.nn.sigmoid(gate_pre)
    activated = gate_pre * sigmoid_gate
    hidden = (activated * up_pre).astype(jnp.bfloat16)
    hidden_grad = jnp.dot(grads_in, down_w.T, preferred_element_type=jnp.float32)
    slope = sigmoid_gate * (1.0 + gate_pre * (1.0 - sigmoid_gate))
    gate_grad = (hidden_grad * up_pre * slope).astype(jnp.bfloat16)
    up_grad = (hidden_grad * activated).astype(jnp.bfloat16)
    grad_down = jnp.dot(hidden.T, grads_in, preferred_element_type=jnp.float32).astype(jnp.bfloat16)
    grad_gate_w = jnp.dot(saved.T, gate_grad, preferred_element_type=jnp.float32).astype(jnp.bfloat16)
    grad_up_w = jnp.dot(saved.T, up_grad, preferred_element_type=jnp.float32).astype(jnp.bfloat16)
    row_value = jnp.dot(gate_grad, gate_w.T, preferred_element_type=jnp.float32) + jnp.dot(up_grad, up_w.T, preferred_element_type=jnp.float32)
    row_grad = row_value.astype(jnp.bfloat16)
    return (grad_gate_w, grad_up_w, grad_down, row_grad)

def reference(out_cotangent, routes, route_weights, expert_rows, w_gate, w_up, w_down, out_weight, values, keys, queries, log_decay, gate_input):
    model_width = out_cotangent.shape[1]
    pair_count = TOK_DEV * TOP
    flat_routes = routes.reshape(N_SP, pair_count)
    expert_ids = jnp.arange(EXPERTS, dtype=jnp.int32)
    onehot = (flat_routes[:, :, None] == expert_ids[None, None, :]).astype(jnp.int32)
    pair_rank = lax.optimization_barrier(jnp.sum(jnp.cumsum(onehot, axis=1) * onehot, axis=2)) - 1
    pair_slot = (jnp.arange(N_SP, dtype=jnp.int32)[:, None] * CAP + pair_rank).astype(jnp.int32)
    scaled = (route_weights[:, :, None] * out_cotangent[:, None, :].astype(jnp.float32)).astype(jnp.bfloat16)
    scaled = scaled.reshape(N_SP, pair_count, model_width)
    dispatched = jnp.zeros((EXPERTS, SLOTS, model_width), jnp.bfloat16).at[flat_routes, pair_slot].set(scaled)
    grad_w_gate, grad_w_up, grad_w_down, row_grads = lax.map(expert_backward, (expert_rows, dispatched, w_gate, w_up, w_down))
    returned = row_grads[flat_routes, pair_slot].reshape(SEQUENCE_TOKENS, TOP, model_width)
    grad_residual = out_cotangent.astype(jnp.float32) + lax.optimization_barrier(jnp.sum(returned.astype(jnp.float32), axis=1))
    residual_low = grad_residual.astype(jnp.bfloat16)
    zero_state = jnp.zeros((MIXER_HEADS, HEAD_DIM, STATE), jnp.float32)

    def forward(value_f, key_f, query_f, decay_f):
        return mixer_scan(value_f, key_f, query_f, decay_f, zero_state)[0]
    mixer_y, pull_back = jax.vjp(forward, values.astype(jnp.float32), keys.astype(jnp.float32), queries.astype(jnp.float32), log_decay)
    gate_f = gate_input.astype(jnp.float32)
    sigmoid_gate = jax.nn.sigmoid(gate_f)
    activated = gate_f * sigmoid_gate
    slope = sigmoid_gate * (1.0 + gate_f * (1.0 - sigmoid_gate))
    mixed = (mixer_y * activated).astype(jnp.bfloat16)
    mixed_grad = jnp.dot(residual_low, out_weight, preferred_element_type=jnp.float32)
    grad_out_weight = jnp.dot(residual_low.T, mixed, preferred_element_type=jnp.float32)
    grad_gate = mixed_grad * mixer_y * slope
    y_grad = mixed_grad * activated
    grad_values, grad_keys, grad_queries, grad_decay = pull_back(y_grad)
    return (grad_w_gate, grad_w_up, grad_w_down, grad_out_weight, grad_residual, grad_values, grad_keys, grad_queries, grad_decay, grad_gate)
```

```python
import jax
import jax.numpy as jnp
from jax import lax
from jax.experimental import pallas as pl
from jax.experimental.pallas import tpu as pltpu
from jax.sharding import PartitionSpec as P

STATE = 128

HIGHEST = lax.Precision.HIGHEST
BF16 = jnp.bfloat16
F32 = jnp.float32


def dot_f32(a, b, dims):
    return lax.dot_general(a, b, (dims, ((), ())), preferred_element_type=F32)


def gather_columns(own, axis):
    count = lax.axis_size(axis)
    if count != 4:
        return lax.all_gather(own, axis, axis=1, tiled=True)
    across = lax.ppermute(own, axis, [(s, s ^ 2) for s in range(count)])
    near = lax.ppermute(own, axis, [(s, s ^ 1) for s in range(count)])
    far = lax.ppermute(across, axis, [(s, s ^ 1) for s in range(count)])
    place = lax.axis_index(axis)
    odd = (place % 2) == 1
    upper = (place // 2) == 1
    same_even, same_odd = jnp.where(odd, near, own), jnp.where(odd, own, near)
    other_even, other_odd = jnp.where(odd, far, across), jnp.where(odd, across, far)
    return jnp.concatenate(
        [
            jnp.where(upper, other_even, same_even),
            jnp.where(upper, other_odd, same_odd),
            jnp.where(upper, same_even, other_even),
            jnp.where(upper, same_odd, other_odd),
        ],
        axis=1,
    )


def carry_kernel(count, rows, reverse):
    def body(decay_ref, part_ref, out_ref):
        state = jnp.zeros((rows, part_ref.shape[1]), F32)
        for step in range(count):
            at = count - 1 - step if reverse else step
            span = pl.ds(at * rows, rows)
            out_ref[span, :] = state.astype(BF16)
            state = state * decay_ref[span, :] + part_ref[span, :].astype(F32)

    return body


def carried(part, row_decay, axis, reverse):
    count = lax.axis_size(axis)
    total_rows, width = part.shape
    rows = total_rows // count
    seen = lax.all_to_all(part.astype(BF16), axis, split_axis=0, concat_axis=0, tiled=True)
    states = pl.pallas_call(
        carry_kernel(count, rows, reverse),
        out_shape=jax.ShapeDtypeStruct((total_rows, width), BF16),
    )(row_decay, seen)
    return lax.all_to_all(states, axis, split_axis=0, concat_axis=0, tiled=True)


def within_kernel(repeat, head_dim):
    def body(v_ref, k_ref, q_ref, col_ref, row_ref, up_ref, g_ref, s_ref, ones_ref,
             gv_ref, gk_ref, gq_ref, rowsum_ref, colsum_ref):
        span = v_ref.shape[0]
        keys, queries = k_ref[...], q_ref[...]
        inner = dot_f32(queries, keys, ((1,), (1,)))
        lower = lax.broadcasted_iota(jnp.int32, (span, span), 0) >= lax.broadcasted_iota(
            jnp.int32, (span, span), 1
        )
        inner_grad = jnp.zeros((span, span), F32)
        state = s_ref[...]
        scaled = g_ref[...] * up_ref[...]
        reach = dot_f32(queries, state, ((1,), (1,)))
        carry_sum = jnp.dot(scaled * reach, ones_ref[...], precision=HIGHEST)
        row_sums = []
        for head in range(repeat):
            cols = pl.ds(head * head_dim, head_dim)
            segment = col_ref[0, :, head:head + 1] - row_ref[0, head:head + 1, :]
            weights = jnp.exp(jnp.where(lower, segment, -jnp.inf))
            grad = g_ref[:, cols].astype(BF16)
            from_pairs = dot_f32(grad, v_ref[:, cols], ((1,), (1,))) * weights
            inner_grad = inner_grad + from_pairs
            gv_ref[:, cols] = dot_f32((inner * weights).astype(BF16), grad, ((0,), (0,)))
            pair_grad = from_pairs * inner
            row_sums.append(jnp.sum(pair_grad, axis=1, keepdims=True))
            colsum_ref[0, head:head + 1, :] = jnp.sum(pair_grad, axis=0, keepdims=True)
        rowsum_ref[0] = jnp.concatenate(row_sums, axis=1) + carry_sum
        low = inner_grad.astype(BF16)
        gq_ref[...] = dot_f32(low, keys, ((1,), (0,))) + dot_f32(
            scaled.astype(BF16), state, ((1,), (0,))
        )
        gk_ref[...] = dot_f32(low, queries, ((0,), (0,)))

    return body


def leaving_kernel(repeat, head_dim):
    def body(v_ref, k_ref, end_ref, total_ref, r_ref, s_ref, ones_ref, gv_in, gk_in, dec_in,
             gv_ref, gk_ref, dec_ref):
        span = v_ref.shape[0]
        later = r_ref[...]
        value_end = v_ref[...].astype(F32) * end_ref[...]
        back = dot_f32(k_ref[...], later, ((1,), (1,)))
        gv_ref[...] = gv_in[...] + end_ref[...] * back
        gk_ref[...] = gk_in[...] + dot_f32(value_end.astype(BF16), later, ((1,), (0,)))
        per_token = jnp.dot(value_end * back, ones_ref[...], precision=HIGHEST)
        before = (
            lax.broadcasted_iota(jnp.int32, (span, span), 0)
            > lax.broadcasted_iota(jnp.int32, (span, span), 1)
        ).astype(F32)
        through = jnp.dot(before, per_token, precision=HIGHEST)
        kept = later.astype(F32) * s_ref[...].astype(F32)
        kept = jnp.sum(kept.reshape(repeat, head_dim, kept.shape[1]), axis=1)
        kept = lax.dot_general(
            jnp.ones((1, kept.shape[1]), F32), kept, (((1,), (1,)), ((), ())), precision=HIGHEST
        )
        dec_ref[0] = dec_in[0] + through + total_ref[0] * kept

    return body


def shards(
    out_cotangent,
    routes,
    route_weights,
    expert_rows,
    w_gate,
    w_up,
    w_down,
    out_weight,
    values,
    keys,
    queries,
    log_decay,
    gate_input,
):
    sp_size = lax.axis_size("sp")
    tp_size = lax.axis_size("tp")
    sp_place = lax.axis_index("sp")
    tok_count, model_width = out_cotangent.shape
    top = routes.shape[1]
    local_experts = w_gate.shape[0]
    slot_count = expert_rows.shape[1]
    capacity = slot_count // sp_size
    experts_all = local_experts * sp_size
    columns = model_width // tp_size
    pair_count = tok_count * top
    row_columns = expert_rows.shape[2]
    full_rows = gather_columns(
        expert_rows.reshape(local_experts * slot_count, row_columns), "tp"
    ).reshape(local_experts, slot_count, row_columns * tp_size)
    all_weight = lax.all_gather(out_weight, "sp", axis=0, tiled=True)

    pair_list = routes.reshape(-1)
    onehot = (pair_list[:, None] == jnp.arange(experts_all, dtype=jnp.int32)[None, :]).astype(BF16)
    earlier = (jnp.arange(pair_count)[:, None] > jnp.arange(pair_count)[None, :]).astype(BF16)
    pair_rank = jnp.sum(
        jnp.dot(earlier, onehot, preferred_element_type=F32) * onehot.astype(F32), axis=1
    ).astype(jnp.int32)
    target = pair_list * capacity + pair_rank
    placed = (
        target[None, :] == jnp.arange(experts_all * capacity, dtype=jnp.int32)[:, None]
    ).astype(BF16)
    own_columns = lax.dynamic_slice_in_dim(
        out_cotangent, lax.axis_index("tp") * columns, columns, 1
    ).astype(F32)
    scaled = (route_weights[:, :, None] * own_columns[:, None, :]).astype(BF16)
    outgoing = jnp.dot(
        placed, scaled.reshape(pair_count, columns), preferred_element_type=F32
    ).astype(BF16)
    arrived = lax.all_to_all(outgoing, "sp", split_axis=0, concat_axis=0, tiled=True)
    arrived = jnp.moveaxis(arrived.reshape(sp_size, local_experts, capacity, columns), 0, 1)
    arrived = gather_columns(
        arrived.reshape(local_experts * slot_count, columns), "tp"
    ).reshape(local_experts, slot_count, model_width)

    head_count = log_decay.shape[1]
    groups = keys.shape[1] // STATE
    head_dim = values.shape[1] // head_count
    repeat = head_count // groups
    state_rows = head_count * head_dim
    key_f = keys.astype(F32).reshape(tok_count, groups, STATE)
    query_f = queries.astype(F32).reshape(tok_count, groups, STATE)
    upto = jnp.arange(tok_count)[:, None] >= jnp.arange(tok_count)[None, :]
    cumulative = jnp.dot(upto.astype(F32), log_decay, precision=HIGHEST)
    last = cumulative[-1]
    decay_total = jnp.exp(last)
    from_start = jnp.repeat(jnp.exp(cumulative), head_dim, axis=1)
    to_end = jnp.repeat(jnp.exp(last[None, :] - cumulative), head_dim, axis=1)
    all_decay = lax.all_gather(decay_total, "sp")
    own_part = state_rows // sp_size
    row_decay = lax.dynamic_slice_in_dim(
        jnp.repeat(all_decay, head_dim, axis=1), sp_place * own_part, own_part, 1
    ).reshape(state_rows)
    row_decay = jnp.broadcast_to(row_decay[:, None], (state_rows, STATE))
    value_f = values.astype(F32)
    own_state = jnp.einsum(
        "sgn,sgx->gxn",
        key_f,
        (value_f * to_end).reshape(tok_count, groups, repeat * head_dim),
        precision=HIGHEST,
    ).reshape(state_rows, STATE)
    entry_state = carried(own_state, row_decay, "sp", False)
    segment = cumulative[:, None, :] - cumulative[None, :, :]
    weights = jnp.exp(jnp.where(upto[:, :, None], segment, -jnp.inf)).reshape(
        tok_count, tok_count, groups, repeat
    )
    inner_prod = jnp.einsum("tgn,sgn->tsg", query_f, key_f, precision=HIGHEST)
    within = jnp.einsum(
        "tsgr,sgrp->tgrp",
        inner_prod[:, :, :, None] * weights,
        value_f.reshape(tok_count, groups, repeat, head_dim),
        precision=HIGHEST,
    ).reshape(tok_count, state_rows)
    reach = jnp.einsum(
        "tgn,gxn->tgx",
        query_f,
        entry_state.astype(F32).reshape(groups, repeat * head_dim, STATE),
        precision=HIGHEST,
    ).reshape(tok_count, state_rows)
    mixer_y = within + reach * from_start
    gate_f = gate_input.astype(F32)
    gate_sigmoid = jax.nn.sigmoid(gate_f)
    gate_active = gate_f * gate_sigmoid
    gate_slope = gate_sigmoid * (1.0 + gate_f * (1.0 - gate_sigmoid))
    mixed = (mixer_y * gate_active).astype(BF16)
    all_mixed = lax.all_gather(mixed, "sp", axis=0, tiled=True)

    gate_pre = jnp.einsum("esd,edf->esf", full_rows, w_gate, preferred_element_type=F32)
    up_pre = jnp.einsum("esd,edf->esf", full_rows, w_up, preferred_element_type=F32)
    sigmoid_gate = jax.nn.sigmoid(gate_pre)
    activated = gate_pre * sigmoid_gate
    hidden = (activated * up_pre).astype(BF16)
    hidden_grad = jnp.einsum("esd,efd->esf", arrived, w_down, preferred_element_type=F32)
    slope = sigmoid_gate * (1.0 + gate_pre * (1.0 - sigmoid_gate))
    gate_grad = (hidden_grad * up_pre * slope).astype(BF16)
    up_grad = (hidden_grad * activated).astype(BF16)
    partial_value = jnp.einsum("esf,edf->esd", gate_grad, w_gate, preferred_element_type=F32)
    partial_value = partial_value + jnp.einsum(
        "esf,edf->esd", up_grad, w_up, preferred_element_type=F32
    )
    partial_value = partial_value.astype(BF16).reshape(
        local_experts * slot_count, tp_size, columns
    )
    partial_value = jnp.moveaxis(partial_value, 1, 0)
    partial_value = lax.all_to_all(partial_value, "tp", split_axis=0, concat_axis=0, tiled=True)
    summed = jnp.sum(partial_value.astype(F32), axis=0).astype(BF16)
    send_back = jnp.moveaxis(summed.reshape(local_experts, sp_size, capacity, columns), 1, 0)
    returned = lax.all_to_all(
        send_back.reshape(experts_all * capacity, columns),
        "sp",
        split_axis=0,
        concat_axis=0,
        tiled=True,
    )
    taken = jnp.sum(placed.reshape(-1, tok_count, top).astype(F32), axis=2).astype(BF16)
    grad_residual = own_columns + dot_f32(taken, returned, ((0,), (0,)))
    residual_low = lax.all_gather(grad_residual.astype(BF16), "tp", axis=1, tiled=True)

    mixed_grad = jnp.dot(residual_low, all_weight, preferred_element_type=F32)
    y_grad = mixed_grad * gate_active
    grad_gate = mixed_grad * mixer_y * gate_slope
    reached_state = jnp.einsum(
        "tgn,tgx->gxn",
        query_f,
        (y_grad * from_start).reshape(tok_count, groups, repeat * head_dim),
        precision=HIGHEST,
    ).reshape(state_rows, STATE)
    later_state = carried(reached_state, row_decay, "sp", True)
    head_sum = (
        jnp.arange(repeat * head_dim)[:, None] // head_dim == jnp.arange(repeat)[None, :]
    ).astype(F32)
    wide = repeat * head_dim
    wide_spec = pl.BlockSpec((tok_count, wide), lambda g: (0, g))
    state_spec = pl.BlockSpec((tok_count, STATE), lambda g: (0, g))
    rows_spec = pl.BlockSpec((wide, STATE), lambda g: (g, 0))
    col_spec = pl.BlockSpec((1, tok_count, repeat), lambda g: (g, 0, 0))
    row_spec = pl.BlockSpec((1, repeat, tok_count), lambda g: (g, 0, 0))
    one_spec = pl.BlockSpec((1, 1, repeat), lambda g: (g, 0, 0))
    sum_spec = pl.BlockSpec((wide, repeat), lambda g: (0, 0))
    wide_shape = jax.ShapeDtypeStruct((tok_count, state_rows), F32)
    state_shape = jax.ShapeDtypeStruct((tok_count, groups * STATE), F32)
    col_shape = jax.ShapeDtypeStruct((groups, tok_count, repeat), F32)
    row_shape = jax.ShapeDtypeStruct((groups, repeat, tok_count), F32)
    cum_col = jnp.moveaxis(cumulative.reshape(tok_count, groups, repeat), 1, 0)
    cum_row = cumulative.T.reshape(groups, repeat, tok_count)
    gv_within, gk_within, grad_queries, row_sums, col_sums = pl.pallas_call(
        within_kernel(repeat, head_dim),
        grid=(groups,),
        in_specs=[wide_spec, state_spec, state_spec, col_spec, row_spec, wide_spec, wide_spec,
                  rows_spec, sum_spec],
        out_specs=[wide_spec, state_spec, state_spec, col_spec, row_spec],
        out_shape=[wide_shape, state_shape, state_shape, col_shape, row_shape],
    )(values, keys, queries, cum_col, cum_row, from_start, y_grad, entry_state, head_sum)
    decay_now = row_sums - jnp.swapaxes(col_sums, 1, 2)
    decay_within = jnp.einsum("ts,gtr->gsr", upto.astype(F32), decay_now, precision=HIGHEST)
    grad_values, grad_keys, decay_grad = pl.pallas_call(
        leaving_kernel(repeat, head_dim),
        grid=(groups,),
        in_specs=[wide_spec, state_spec, wide_spec, one_spec, rows_spec, rows_spec, sum_spec,
                  wide_spec, state_spec, col_spec],
        out_specs=[wide_spec, state_spec, col_spec],
        out_shape=[wide_shape, state_shape, col_shape],
    )(
        values, keys, to_end, decay_total.reshape(groups, 1, repeat), later_state, entry_state,
        head_sum, gv_within, gk_within, decay_within,
    )
    grad_decay = jnp.moveaxis(decay_grad, 0, 1).reshape(tok_count, head_count)

    out_rows = out_weight.shape[0]
    residual_rows = jnp.moveaxis(residual_low.reshape(tok_count, sp_size, out_rows), 1, 0)
    residual_rows = lax.all_to_all(
        residual_rows.reshape(sp_size * tok_count, out_rows),
        "sp",
        split_axis=0,
        concat_axis=0,
        tiled=True,
    )
    grad_out_weight = dot_f32(residual_rows, all_mixed, ((0,), (0,)))
    grad_w_down = jnp.einsum("esf,esd->efd", hidden, arrived, preferred_element_type=F32)
    grad_w_gate = jnp.einsum("esd,esf->edf", full_rows, gate_grad, preferred_element_type=F32)
    grad_w_up = jnp.einsum("esd,esf->edf", full_rows, up_grad, preferred_element_type=F32)
    return (
        grad_w_gate.astype(BF16),
        grad_w_up.astype(BF16),
        grad_w_down.astype(BF16),
        grad_out_weight,
        grad_residual,
        grad_values,
        grad_keys,
        grad_queries,
        grad_decay,
        grad_gate,
    )


def solution(mesh):
    return jax.shard_map(
        shards,
        mesh=mesh,
        in_specs=(
            P("sp", None),
            P("sp", None),
            P("sp", None),
            P("sp", None, "tp"),
            P("sp", None, "tp"),
            P("sp", None, "tp"),
            P("sp", "tp", None),
            P("sp", "tp"),
            P("sp", "tp"),
            P("sp", "tp"),
            P("sp", "tp"),
            P("sp", "tp"),
            P("sp", "tp"),
        ),
        out_specs=(
            P("sp", None, "tp"),
            P("sp", None, "tp"),
            P("sp", "tp", None),
            P("sp", "tp"),
            P("sp", "tp"),
            P("sp", "tp"),
            P("sp", "tp"),
            P("sp", "tp"),
            P("sp", "tp"),
            P("sp", "tp"),
        ),
        check_vma=False,
    )
```
